32 devices in a mesh: rep: 2 (over y), fs: 4 (over z), tp: 4 (over x, core).
Axes of the slice: x: 2, y: 2, z: 4, core: 2. Of those that a mesh axis runs over, the one named last changes fastest.
Arguments:
- activations: bfloat16 [2048, 4096], P(None, ('rep', 'fs')), may hold values from -60 to 60
- w_mix_in: bfloat16 [2048, 1024], P('fs', 'tp'), may hold values from -0.125 to 0.125
- w_mix_out: bfloat16 [2048, 1024], P('fs', 'tp'), may hold values from -0.1875 to 0.1875
- w_gate: bfloat16 [2048, 2816], P('fs', 'tp'), may hold values from -0.125 to 0.125
- w_up: bfloat16 [2048, 2816], P('fs', 'tp'), may hold values from -0.125 to 0.125
- w_down: bfloat16 [2048, 2816], P('fs', 'tp'), may hold values from -0.109375 to 0.109375
- pool_scale: float32 [1024], replicated, may hold values from 0.1 to 1.9
- gain_mix: float32 [2048], replicated, may hold values from 0.1 to 1.9
- gain_ffn: float32 [2048], replicated, may hold values from 0.1 to 1.9
- gain_out: float32 [2048], replicated, may hold values from 0.1 to 1.9
Outputs:
- normalized: bfloat16 [2048, 4096], P('tp', ('rep', 'fs'))
The draws below stay inside these ranges and needn't reach their ends.
All inputs are finite; a program needn't handle non-finite values.
Results may differ from the reference program's by a relative error of at most 0.014.
Values may be sent and summed in bfloat16 or wider, within the bound.
No kernel may reach another device: no remote copies, remote signals or barrier semaphores. Data moves between devices by JAX's collectives and lax.ppermute only.
A program may use at most 64 MiB of HBM per device.

```python
import jax
import jax.numpy as jnp
from jax import lax

D = 2048
BRANCH = 1024
FF = 2816
POOL_GROUP = 256
SEQ_LEN = 256
TOKENS = 4096
N_TP = 4


def draw_activations(key, part):
    key_rough, key_noise = jax.random.split(key, 2)
    feature_place = jnp.arange(D, dtype=jnp.float32)[:, None] / D
    rough = jax.random.uniform(key_rough, (D, 1), jnp.float32, -0.3, 0.3)
    feature_scale = 0.5 * jnp.exp(jnp.log(8.0) * feature_place + rough)
    values = jnp.clip(jax.random.normal(key_noise, (D, TOKENS), jnp.float32), -6.0, 6.0)
    return jnp.clip(values * feature_scale, -60.0, 60.0).astype(jnp.bfloat16)


def levels(own_key, shape, shards, smallest, top_value):
    def one(axis_at, blocks):
        draws = jax.random.uniform(jax.random.fold_in(jax.random.fold_in(own_key, 6), axis_at), (blocks,), jnp.float32, smallest / len(shards), top_value / len(shards))
        return jnp.repeat(jnp.exp(draws), shape[axis_at] // blocks).reshape((-1,) + (1,) * (len(shape) - axis_at - 1))

    gain = one(*shards[0])
    for cut in shards[1:]:
        gain = gain * one(*cut)
    return gain


def gaussian(rng, shape, scale, reach, shards=(), kind=jnp.bfloat16):
    drawn = scale * jax.random.normal(rng, shape, jnp.float32)
    if shards:
        drawn = drawn * levels(rng, shape, shards, -0.22, 0.18)
    return jnp.clip(drawn, -reach, reach).astype(kind)


def setup_inputs(seed: int = 0) -> dict:
    key_list = jax.random.split(jax.random.key(seed), 11)
    activations = draw_activations(jax.random.fold_in(key_list[10], 71), 0)
    w_mix_in = gaussian(key_list[1], (D, BRANCH), D ** -0.5, 0.125, ((0, 4), (1, 4)))
    w_mix_out = gaussian(key_list[2], (D, BRANCH), BRANCH ** -0.5, 0.1875, ((0, 4), (1, 4)))
    w_gate = gaussian(key_list[3], (D, FF), D ** -0.5, 0.125, ((0, 4), (1, 4)))
    w_up = gaussian(key_list[4], (D, FF), D ** -0.5, 0.125, ((0, 4), (1, 4)))
    w_down = gaussian(key_list[5], (D, FF), FF ** -0.5, 0.109375, ((0, 4), (1, 4)))
    pool_scale = jnp.clip(1.0 + 0.18 * jax.random.normal(key_list[6], (BRANCH,), jnp.float32), 0.1, 1.9)
    gain_mix = jnp.clip(1.0 + 0.18 * jax.random.normal(key_list[7], (D,), jnp.float32), 0.1, 1.9)
    gain_ffn = jnp.clip(1.0 + 0.18 * jax.random.normal(key_list[8], (D,), jnp.float32), 0.1, 1.9)
    gain_out = jnp.clip(1.0 + 0.18 * jax.random.normal(key_list[9], (D,), jnp.float32), 0.1, 1.9)
    return {"activations": activations, "w_mix_in": w_mix_in, "w_mix_out": w_mix_out, "w_gate": w_gate, "w_up": w_up, "w_down": w_down, "pool_scale": pool_scale, "gain_mix": gain_mix, "gain_ffn": gain_ffn, "gain_out": gain_out}


EPS = 1e-06
WINDOWS = (2, 4, 8, 16)

def rms_factor(stream):
    return lax.rsqrt(lax.optimization_barrier(jnp.mean(stream * stream, axis=0, keepdims=True)) + EPS)

def pool_tokens(inputs, group_of):
    channels = inputs.shape[0]
    values = inputs.astype(jnp.float32).reshape(channels, -1, SEQ_LEN)
    sequences = values.shape[1]
    running = jnp.concatenate([jnp.zeros((channels, sequences, 1), jnp.float32), jnp.cumsum(values, axis=-1)], axis=-1)
    places = jnp.arange(SEQ_LEN, dtype=jnp.int32)
    pooled_sum = jnp.zeros_like(values)
    for group_id, window in enumerate(WINDOWS):
        behind = window // 2
        onward = window - behind
        upper_sum = jnp.concatenate([running, jnp.repeat(running[..., -1:], onward, axis=-1)], axis=-1)[..., onward:onward + SEQ_LEN]
        lower_sum = jnp.concatenate([jnp.zeros((channels, sequences, behind), jnp.float32), running], axis=-1)[..., :SEQ_LEN]
        counts = (jnp.minimum(places + onward, SEQ_LEN) - jnp.maximum(places - behind, 0)).astype(jnp.float32)
        window_mean = (upper_sum - lower_sum) / counts
        pooled_sum = pooled_sum + jnp.where((group_of == group_id)[:, None, None], window_mean, 0.0)
    return (pooled_sum - values).reshape(channels, -1)

def block_sum(weights, acts, blocks):
    width = acts.shape[0] // blocks
    stacked_weights = jnp.transpose(weights.reshape(weights.shape[0], blocks, width), (1, 0, 2))
    stacked_acts = acts.reshape(blocks, width, acts.shape[1])

    def add_block(carry, pair):
        term = jnp.dot(pair[0], pair[1], preferred_element_type=jnp.float32).astype(jnp.bfloat16)
        term = lax.optimization_barrier(term)
        return (carry + term.astype(jnp.float32), None)
    start = jnp.zeros((weights.shape[0], acts.shape[1]), jnp.float32)
    total, _ = lax.scan(add_block, start, (stacked_weights, stacked_acts))
    return total

def reference(activations, w_mix_in, w_mix_out, w_gate, w_up, w_down, pool_scale, gain_mix, gain_ffn, gain_out):
    stream = activations.astype(jnp.float32)
    normed = (stream * rms_factor(stream) * gain_mix[:, None]).astype(jnp.bfloat16)
    inputs = jnp.dot(w_mix_in.T, normed, preferred_element_type=jnp.float32).astype(jnp.bfloat16)
    group_of = (jnp.arange(BRANCH, dtype=jnp.int32) // POOL_GROUP).astype(jnp.int32)
    pooled = (pool_tokens(inputs, group_of) * pool_scale[:, None]).astype(jnp.bfloat16)
    mixed = block_sum(w_mix_out, pooled, N_TP)
    after_mix = lax.optimization_barrier((stream + mixed).astype(jnp.bfloat16)).astype(jnp.float32)
    normed_two = (after_mix * rms_factor(after_mix) * gain_ffn[:, None]).astype(jnp.bfloat16)
    gate = jnp.dot(w_gate.T, normed_two, preferred_element_type=jnp.float32)
    upward = jnp.dot(w_up.T, normed_two, preferred_element_type=jnp.float32)
    hidden = (jax.nn.silu(gate) * upward).astype(jnp.bfloat16)
    ffn_out = block_sum(w_down, hidden, N_TP)
    final = after_mix + ffn_out
    return (final * rms_factor(final) * gain_out[:, None]).astype(jnp.bfloat16)
```

```python
import jax
import jax.numpy as jnp
from jax import lax
from jax.sharding import PartitionSpec as P

POOL_GROUP = 256
SEQ_LEN = 256


EPS = 1e-06
WINDOWS = (2, 4, 8, 16)


def rms_factor(stream):
    return lax.rsqrt(jnp.mean(stream * stream, axis=0, keepdims=True) + EPS)


def pool_group(inputs, group_id):
    channels = inputs.shape[0]
    window = jnp.left_shift(WINDOWS[0], group_id)
    behind = window // 2
    onward = window - behind
    source = lax.broadcasted_iota(jnp.int32, (SEQ_LEN, SEQ_LEN), 0)
    place = lax.broadcasted_iota(jnp.int32, (SEQ_LEN, SEQ_LEN), 1)
    band = ((source >= place - behind) & (source < place + onward)).astype(jnp.bfloat16)
    places = jnp.arange(SEQ_LEN, dtype=jnp.int32)
    counts = (jnp.minimum(places + onward, SEQ_LEN) - jnp.maximum(places - behind, 0)).astype(
        jnp.float32
    )
    values = inputs.reshape(channels, -1, SEQ_LEN)
    sums = lax.dot_general(
        values, band, (((2,), (0,)), ((), ())), preferred_element_type=jnp.float32
    )
    return (sums / counts - values.astype(jnp.float32)).reshape(channels, -1)


def pool_tokens(inputs, first_channel):
    channels = inputs.shape[0]
    width = min(channels, POOL_GROUP)
    return jnp.concatenate(
        [
            pool_group(inputs[at : at + width], (first_channel + at) // POOL_GROUP)
            for at in range(0, channels, width)
        ],
        axis=0,
    )


def contract_first(weights, acts):
    return lax.dot_general(
        weights, acts, (((0,), (0,)), ((), ())), preferred_element_type=jnp.float32
    )


def dot(a, b):
    return jnp.dot(a, b, preferred_element_type=jnp.float32)


def on_device_general(
    activations, w_mix_in, w_mix_out, w_gate, w_up, w_down, pool_scale, gain_mix, gain_ffn, gain_out
):
    group_size = lax.axis_size("tp")
    group_rank = lax.axis_index("tp")
    features = activations.shape[0]
    feature_share = features // group_size
    feature_start = group_rank * feature_share
    stream = activations.astype(jnp.float32)
    normed = (stream * rms_factor(stream) * gain_mix[:, None]).astype(jnp.bfloat16)
    in_full = lax.all_gather(w_mix_in, "fs", axis=0, tiled=True)
    out_full = lax.all_gather(w_mix_out, "fs", axis=0, tiled=True)
    inputs = contract_first(in_full, normed).astype(jnp.bfloat16)
    channel_share = w_mix_in.shape[1]
    scale_own = lax.dynamic_slice_in_dim(pool_scale, group_rank * channel_share, channel_share)
    pooled = (pool_tokens(inputs, group_rank * channel_share) * scale_own[:, None]).astype(
        jnp.bfloat16
    )
    mixed = lax.psum(dot(out_full, pooled).astype(jnp.bfloat16), "tp").astype(jnp.float32)
    after_mix = lax.optimization_barrier((stream + mixed).astype(jnp.bfloat16)).astype(jnp.float32)
    normed_two = (after_mix * rms_factor(after_mix) * gain_ffn[:, None]).astype(jnp.bfloat16)
    after_own = lax.dynamic_slice_in_dim(after_mix, feature_start, feature_share, 0)
    gate_full = lax.all_gather(w_gate, "fs", axis=0, tiled=True)
    up_full = lax.all_gather(w_up, "fs", axis=0, tiled=True)
    down_full = lax.all_gather(w_down, "fs", axis=0, tiled=True)
    gate = contract_first(gate_full, normed_two)
    upward = contract_first(up_full, normed_two)
    hidden = (jax.nn.silu(gate) * upward).astype(jnp.bfloat16)
    ffn_own = lax.psum_scatter(
        dot(down_full, hidden).astype(jnp.bfloat16), "tp", scatter_dimension=0, tiled=True
    ).astype(jnp.float32)
    final_own = after_own + ffn_own
    final_squares = lax.psum(jnp.sum(final_own * final_own, axis=0), "tp")
    final_factor = lax.rsqrt(final_squares / features + EPS)
    gain_last = lax.dynamic_slice_in_dim(gain_out, feature_start, feature_share)
    return (final_own * final_factor[None, :] * gain_last[:, None]).astype(jnp.bfloat16)


def swap(x, axis, bit):
    size = lax.axis_size(axis)
    return lax.ppermute(x, axis, [(i, i ^ bit) for i in range(size)])


def line_gather(mine):
    two = swap(mine, "fs", 2)
    one = swap(mine, "fs", 1)
    middle = lax.ppermute(mine, "fs", [(1, 2), (2, 1)])
    ends = lax.ppermute(two, "fs", [(2, 3), (1, 0)])
    z = lax.axis_index("fs")
    three = jnp.where((z == 1) | (z == 2), middle, ends)
    return one, two, three


def on_device_lines(
    activations, w_mix_in, w_mix_out, w_gate, w_up, w_down, pool_scale, gain_mix, gain_ffn, gain_out
):
    y, z, t = lax.axis_index("rep"), lax.axis_index("fs"), lax.axis_index("tp")
    core, x = t & 1, t >> 1
    blocks = lax.axis_size("fs")
    features, tokens = activations.shape
    rows = features // blocks
    first = y == 0

    def own_order(a):
        return jnp.concatenate(
            [lax.dynamic_slice_in_dim(a, (z ^ k) * rows, rows, 0) for k in range(blocks)], axis=0
        )

    mix_mine = jnp.where(first, w_mix_in, w_mix_out)
    mix_rest = line_gather(mix_mine)
    gu_mine = jnp.where(first, w_gate, w_up)
    gu_rest = line_gather(gu_mine)
    half = w_down.shape[1] // 2
    down_mine = lax.dynamic_slice_in_dim(w_down, y * half, half, 1)
    down_rest = line_gather(down_mine)
    mix_other = [swap(p, "rep", 1) for p in mix_rest]
    gu_other = [swap(p, "rep", 1) for p in gu_rest]
    down_other = [swap(p, "rep", 1) for p in down_rest]

    stream_bf = own_order(activations)
    stream = stream_bf.astype(jnp.float32)
    gain_one, gain_two = own_order(gain_mix), own_order(gain_ffn)
    normed = (stream * rms_factor(stream) * gain_one[:, None]).astype(jnp.bfloat16)
    in_full = jnp.concatenate(
        [w_mix_in] + [jnp.where(first, a, b) for a, b in zip(mix_rest, mix_other)], axis=0
    )
    out_full = jnp.concatenate(
        [w_mix_out] + [jnp.where(first, b, a) for a, b in zip(mix_rest, mix_other)], axis=0
    )
    inputs = contract_first(in_full, normed).astype(jnp.bfloat16)
    channel_share = w_mix_in.shape[1]
    scale_own = lax.dynamic_slice_in_dim(pool_scale, t * channel_share, channel_share)
    pooled = (pool_tokens(inputs, t * channel_share) * scale_own[:, None]).astype(jnp.bfloat16)
    term = dot(out_full, pooled).astype(jnp.bfloat16)
    part = features // 2
    keep = lax.dynamic_slice_in_dim(term, core * part, part, 0)
    send = lax.dynamic_slice_in_dim(term, (1 - core) * part, part, 0)
    chip = (keep.astype(jnp.float32) + swap(send, "tp", 1).astype(jnp.float32)).astype(jnp.bfloat16)
    mixed = chip.astype(jnp.float32) + swap(chip, "tp", 2).astype(jnp.float32)
    stream_part = lax.dynamic_slice_in_dim(stream_bf, core * part, part, 0).astype(jnp.float32)
    after_part = (stream_part + mixed).astype(jnp.bfloat16)
    after_other = swap(after_part, "tp", 1)
    low = jnp.where(core == 0, after_part, after_other)
    high = jnp.where(core == 0, after_other, after_part)
    after_bf = lax.optimization_barrier(jnp.concatenate([low, high], axis=0))
    after_mix = after_bf.astype(jnp.float32)
    normed_two = (after_mix * rms_factor(after_mix) * gain_two[:, None]).astype(jnp.bfloat16)

    def block(a, k):
        return a[k * rows : (k + 1) * rows]

    gate = contract_first(w_gate, block(normed_two, 0))
    upward = contract_first(w_up, block(normed_two, 0))
    mine_sum = sum(contract_first(gu_rest[k - 1], block(normed_two, k)) for k in range(1, blocks))
    other_sum = sum(contract_first(gu_other[k - 1], block(normed_two, k)) for k in range(1, blocks))
    gate = gate + jnp.where(first, mine_sum, other_sum)
    upward = upward + jnp.where(first, other_sum, mine_sum)
    hidden = (jax.nn.silu(gate) * upward).astype(jnp.bfloat16)
    hidden_mine = lax.dynamic_slice_in_dim(hidden, y * half, half, 0)
    hidden_other = lax.dynamic_slice_in_dim(hidden, (1 - y) * half, half, 0)
    terms = [dot(w_down, hidden).astype(jnp.bfloat16)]
    for k in range(1, blocks):
        terms.append(
            (dot(down_rest[k - 1], hidden_mine) + dot(down_other[k - 1], hidden_other)).astype(
                jnp.bfloat16
            )
        )
    ffn = jnp.stack(terms).reshape(2, 2, rows, tokens)
    even = core ^ (z & 1)
    keep = lax.dynamic_index_in_dim(ffn, even, 1, keepdims=False)
    send = lax.dynamic_index_in_dim(ffn, 1 - even, 1, keepdims=False)
    chip = (keep.astype(jnp.float32) + swap(send, "tp", 1).astype(jnp.float32)).astype(jnp.bfloat16)
    near = x ^ (z >> 1)
    keep = lax.dynamic_index_in_dim(chip, near, 0, keepdims=False)
    send = lax.dynamic_index_in_dim(chip, 1 - near, 0, keepdims=False)
    ffn_own = keep.astype(jnp.float32) + swap(send, "tp", 2).astype(jnp.float32)
    after_own = lax.dynamic_slice_in_dim(after_bf, (t ^ z) * rows, rows, 0).astype(jnp.float32)
    final_own = after_own + ffn_own
    final_squares = lax.psum(jnp.sum(final_own * final_own, axis=0), "tp")
    final_factor = lax.rsqrt(final_squares / features + EPS)
    gain_last = lax.dynamic_slice_in_dim(gain_out, t * rows, rows)
    return (final_own * final_factor[None, :] * gain_last[:, None]).astype(jnp.bfloat16)


def solution(mesh):
    placed = (
        P(None, ("rep", "fs")),
        P("fs", "tp"),
        P("fs", "tp"),
        P("fs", "tp"),
        P("fs", "tp"),
        P("fs", "tp"),
        P(),
        P(),
        P(),
        P(),
    )
    sizes = mesh.shape
    lines = sizes["fs"] == 4 and sizes["tp"] == 4 and sizes["rep"] == 2
    return jax.shard_map(
        on_device_lines if lines else on_device_general,
        mesh=mesh,
        in_specs=placed,
        out_specs=P("tp", ("rep", "fs")),
        check_vma=False,
    )
```
